32 devices in a mesh: ep: 4 (over y, x), tp: 8 (over z, core).
Axes of the slice: x: 2, y: 2, z: 4, core: 2. Of those that a mesh axis runs over, the one named last changes fastest.
Arguments:
- queries: bfloat16 [4096, 1024], P('ep', 'tp'), may hold values from -600 to 600
- key_rows: bfloat16 [4096, 128], P('ep'), may hold values from -6 to 6
- value_rows: bfloat16 [4096, 128], P('ep'), may hold values from -48 to 48
- sink_logits: float32 [16], P('tp'), may hold values from 2 to 6
- out_weight: bfloat16 [1024, 2048], P('tp'), may hold values from -0.1875 to 0.1875
- moe_rows: bfloat16 [1024, 2048], P(('ep', 'tp')), may hold values from -6 to 6
- moe_gain: float32 [2048], replicated, may hold values from 0.1 to 1.9
- routes: int32 [1024, 2], P(('ep', 'tp')), may hold values from 0 to 3, all different within a row; in each aligned block of 32 rows (0 to 31, 32 to 63, ...) at most 24 rows name the same one
- route_weight: float32 [1024, 2], P(('ep', 'tp')), may hold values from 0.2 to 1
- gate_weight: bfloat16 [4, 2048, 7168], P('ep', None, 'tp'), may hold values from -0.125 to 0.125
- up_weight: bfloat16 [4, 2048, 7168], P('ep', None, 'tp'), may hold values from -0.125 to 0.125
- down_weight: bfloat16 [4, 7168, 2048], P('ep', 'tp'), may hold values from -0.0625 to 0.0625
Outputs:
- mixer_out: bfloat16 [4096, 2048], P(('ep', 'tp'))
- moe_out: bfloat16 [1024, 2048], P(('ep', 'tp'))
The draws below stay inside these ranges and needn't reach their ends.
Inputs may be any that keep to these rules, and one draw needn't show every extreme that they name: `routes`: in each aligned block of 32 rows (the rows of one device) no expert is named more than 24 times, a bound that some block reaches; each row names 2 different experts.
All inputs are finite; a program needn't handle non-finite values.
Results may differ from the reference program's by a relative error of at most 0.02.
Values may be sent and summed in bfloat16 or wider, within the bound.
No kernel may reach another device: no remote copies, remote signals or barrier semaphores. Data moves between devices by JAX's collectives and lax.ppermute only.
A program may use at most 128 MiB of HBM per device.

```python
import math
import jax
import jax.numpy as jnp
import numpy as np
from jax import lax

D = 2048
HEADS = 16
KV_HEADS = 2
HEAD_DIM = 64
WINDOW = 128
FF = 7168
TOP = 2
MOE_DEV = 32
EXPERTS = 4
TOKENS = 4096
MOE_TOKENS = 1024
CAP = 24
N_TP = 8


def draw_queries(key, part):
    base = jax.random.truncated_normal(key, -6.0, 6.0, (TOKENS, HEADS * HEAD_DIM), jnp.float32)
    return base.astype(jnp.bfloat16)


def block_levels(rng, extent, shards, smallest, largest):
    level, own = 1.0, jax.random.fold_in(rng, 6)
    for dim, shards_of in shards:
        draws = jnp.exp(jax.random.uniform(jax.random.fold_in(own, dim), (shards_of,), jnp.float32, smallest / len(shards), largest / len(shards)))
        level = level * jnp.repeat(draws, extent[dim] // shards_of).reshape([-1 if axis == dim else 1 for axis in range(len(extent))])
    return level


def assign_block(own_key, own, number, rows, count, top, most, slope):
    sequence = jax.random.permutation(own_key, count)
    crowded, ordinary = portions_of(count, rows * top, most, slope, True), portions_of(count, rows * top, most, slope, False)
    places = jnp.arange(count)

    def named(tallies, turn):
        used = int((tallies > 0).sum())
        fixed = max(1, used // 4)
        shifted = fixed + (places - fixed + turn * (used - fixed)) % max(1, count - fixed)
        return jnp.zeros((count,), jnp.int32).at[sequence[jnp.where(places < fixed, places, shifted)]].set(jnp.asarray(tallies, jnp.int32))

    tallies = jnp.where(number % 4 == 0, named(crowded, number // 4), named(ordinary, number - number // 4 - 1))
    mixed = jax.random.permutation(jax.random.fold_in(own, 3), count)
    donor, receiver = mixed[0:count // 2 * 2:2], mixed[1:count // 2 * 2:2]
    room = jnp.minimum(tallies[donor] - 1, most - tallies[receiver]) // 2
    room = jnp.where((donor == sequence[0]) | (receiver == sequence[0]) | (tallies[receiver] == 0), 0, jnp.maximum(room, 0))
    shifted = jax.random.randint(jax.random.fold_in(own, 4), (count // 2,), 0, 1 << 20) % (room + 1)
    tallies = tallies.at[donor].add(-shifted).at[receiver].add(shifted)
    members = jnp.searchsorted(jnp.cumsum(tallies), jnp.arange(rows * top), side="right").astype(jnp.int32)
    listing = members.reshape(top, rows).T
    listing = listing[jax.random.permutation(jax.random.fold_in(own, 1), rows)]
    turn = jax.random.randint(jax.random.fold_in(own, 2), (rows, 1), 0, top)
    return jnp.take_along_axis(listing, (jnp.arange(top)[None, :] + turn) % top, axis=1)


def portions_of(amount, total, most, slope, full):
    loads = [(1 << 20) // math.isqrt(standing ** slope) + 1 for standing in range(1, amount + 1)]
    largest = most if full else min(most, max(-(-total // amount), total * loads[0] // sum(loads)))
    least = 1 if total - largest >= amount - 1 else 0
    given, rest = [largest] + [least] * (amount - 1), total - largest - least * (amount - 1)
    while rest > 0:
        free = [i for i in range(1, amount) if given[i] < largest] or [i for i in range(1, amount) if given[i] < most]
        mass, budget = sum([loads[i] for i in free]), rest
        for i in free:
            more = min(most - given[i], max(1, budget * loads[i] // mass), rest)
            given[i] = given[i] + more
            rest = rest - more
    return np.array(given)


def centred(rng, dims, scale, bound, shards=(), kind=jnp.bfloat16):
    level = block_levels(rng, dims, shards, -0.22, 0.18) if shards else 1.0
    drawn = jax.random.normal(rng, dims, jnp.float32) * scale * level
    return jnp.minimum(jnp.maximum(drawn, -bound), bound).astype(kind)


def setup_inputs(seed: int = 0) -> dict:
    seeds = jax.random.split(jax.random.key(seed), 13)
    queries = draw_queries(jax.random.fold_in(seeds[12], 71), 0)
    key_rows = centred(seeds[1], (TOKENS, KV_HEADS * HEAD_DIM), 1.0, 6.0, ((0, 4),))
    value_rows = centred(seeds[2], (TOKENS, KV_HEADS * HEAD_DIM), 8.0, 48.0, ((0, 4),))
    sink_logits = jnp.clip(2.0 + 4.0 * jax.random.uniform(seeds[3], (HEADS,), jnp.float32) ** block_levels(seeds[3], (HEADS,), ((0, 8),), -0.2, 0.2), 2.0, 6.0)
    out_weight = centred(seeds[4], (HEADS * HEAD_DIM, D), (HEADS * HEAD_DIM) ** -0.5, 0.1875, ((0, 8),))
    moe_rows = centred(seeds[5], (MOE_TOKENS, D), 1.0, 6.0, ((0, 32),))
    moe_gain = jnp.clip(1.0 + 0.18 * jax.random.normal(seeds[6], (D,), jnp.float32), 0.1, 1.9)
    routes_keys = jax.random.split(jax.random.fold_in(seeds[7], 1), MOE_TOKENS // MOE_DEV)
    routes_turns = jax.random.permutation(jax.random.fold_in(seeds[7], 3), MOE_TOKENS // MOE_DEV)
    routes = jax.vmap(lambda own, number: assign_block(jax.random.fold_in(seeds[7], 2), own, number, MOE_DEV, EXPERTS, TOP, CAP, 2))(routes_keys, routes_turns).reshape((MOE_TOKENS, TOP))
    route_weight = jnp.clip(0.2 + 0.8 * jax.random.uniform(seeds[8], (MOE_TOKENS, TOP), jnp.float32) ** block_levels(seeds[8], (MOE_TOKENS, TOP), ((0, 32),), -0.2, 0.2), 0.2, 1.0)
    gate_weight = centred(seeds[9], (EXPERTS, D, FF), D ** -0.5, 0.125, ((0, 4), (2, 8)))
    up_weight = centred(seeds[10], (EXPERTS, D, FF), D ** -0.5, 0.125, ((0, 4), (2, 8)))
    down_weight = centred(seeds[11], (EXPERTS, FF, D), FF ** -0.5, 0.0625, ((0, 4), (1, 8)))
    return {"queries": queries, "key_rows": key_rows, "value_rows": value_rows, "sink_logits": sink_logits, "out_weight": out_weight, "moe_rows": moe_rows, "moe_gain": moe_gain, "routes": routes, "route_weight": route_weight, "gate_weight": gate_weight, "up_weight": up_weight, "down_weight": down_weight}


big_negative = -1e+30
norm_eps = 1e-05

def stored_bf16(values):
    return lax.optimization_barrier(values.astype(jnp.bfloat16)).astype(jnp.float32)

def layer_normed(inputs, gain):
    values = inputs.astype(jnp.float32)
    center = values - lax.optimization_barrier(jnp.mean(values, -1, keepdims=True))
    spread = lax.optimization_barrier(jnp.mean(center * center, -1, keepdims=True))
    return (center * lax.rsqrt(spread + norm_eps) * gain).astype(jnp.bfloat16)

def one_head(head_index, queries, key_rows, value_rows, sink_logits):
    total = queries.shape[0]
    blocks = total // WINDOW
    key_head = head_index // (HEADS // KV_HEADS)
    query_cols = lax.dynamic_slice_in_dim(queries, head_index * HEAD_DIM, HEAD_DIM, 1).astype(jnp.float32)
    key_cols = lax.dynamic_slice_in_dim(key_rows, key_head * HEAD_DIM, HEAD_DIM, 1).astype(jnp.float32)
    value_cols = lax.dynamic_slice_in_dim(value_rows, key_head * HEAD_DIM, HEAD_DIM, 1).astype(jnp.float32)
    padding = jnp.zeros((WINDOW, HEAD_DIM), jnp.float32)
    key_ext = jnp.concatenate([padding, key_cols], 0)
    value_ext = jnp.concatenate([padding, value_cols], 0)
    key_blocks = jnp.concatenate([key_ext[:total].reshape(blocks, WINDOW, HEAD_DIM), key_ext[WINDOW:].reshape(blocks, WINDOW, HEAD_DIM)], 1)
    value_blocks = jnp.concatenate([value_ext[:total].reshape(blocks, WINDOW, HEAD_DIM), value_ext[WINDOW:].reshape(blocks, WINDOW, HEAD_DIM)], 1)
    scores = jnp.einsum('nqd,nkd->nqk', query_cols.reshape(blocks, WINDOW, HEAD_DIM), key_blocks) * HEAD_DIM ** (-0.5)
    block_base = jnp.arange(blocks, dtype=jnp.int32)[:, None, None] * WINDOW
    query_pos = block_base + jnp.arange(WINDOW, dtype=jnp.int32)[None, :, None]
    key_pos = block_base - WINDOW + jnp.arange(2 * WINDOW, dtype=jnp.int32)[None, None, :]
    allowed = (key_pos <= query_pos) & (key_pos > query_pos - WINDOW) & (key_pos >= 0)
    masked = jnp.where(allowed, scores, big_negative)
    sink = sink_logits[head_index]
    row_max = jnp.maximum(lax.optimization_barrier(jnp.max(masked, -1)), sink)
    powers = jnp.where(allowed, jnp.exp(masked - row_max[..., None]), 0.0)
    totals = lax.optimization_barrier(jnp.sum(powers, -1)) + jnp.exp(sink - row_max)
    attn_probs = stored_bf16(powers / totals[..., None])
    attended = jnp.einsum('nqk,nkd->nqd', attn_probs, value_blocks)
    return attended.astype(jnp.bfloat16).reshape(total, HEAD_DIM)

def one_expert(inputs):
    expert_rows, gate_mat, up_mat, down_mat = inputs
    gate_val = jnp.dot(expert_rows, gate_mat, preferred_element_type=jnp.float32)
    up_val = jnp.dot(expert_rows, up_mat, preferred_element_type=jnp.float32)
    hidden = (jax.nn.silu(gate_val) * up_val).astype(jnp.bfloat16)
    group_units = FF // N_TP

    def add_group(index, carry):
        first_col = index.astype(jnp.int32) * group_units
        hidden_cols = lax.dynamic_slice_in_dim(hidden, first_col, group_units, 1)
        down_rows = lax.dynamic_slice_in_dim(down_mat, first_col, group_units, 0)
        return carry + stored_bf16(jnp.dot(hidden_cols, down_rows, preferred_element_type=jnp.float32))
    summed = lax.fori_loop(0, N_TP, add_group, jnp.zeros((expert_rows.shape[0], D), jnp.float32))
    return summed.astype(jnp.bfloat16)

def reference(queries, key_rows, value_rows, sink_logits, out_weight, moe_rows, moe_gain, routes, route_weight, gate_weight, up_weight, down_weight):
    total = queries.shape[0]
    per_head = lax.map(lambda index: one_head(index, queries, key_rows, value_rows, sink_logits), jnp.arange(HEADS, dtype=jnp.int32))
    attended = jnp.transpose(per_head, (1, 0, 2)).reshape(total, HEADS * HEAD_DIM)
    group_cols = HEADS // N_TP * HEAD_DIM

    def add_heads(index, carry):
        first_col = index.astype(jnp.int32) * group_cols
        head_cols = lax.dynamic_slice_in_dim(attended, first_col, group_cols, 1)
        proj_rows = lax.dynamic_slice_in_dim(out_weight, first_col, group_cols, 0)
        return carry + stored_bf16(jnp.dot(head_cols, proj_rows, preferred_element_type=jnp.float32))
    mixer_out = lax.fori_loop(0, N_TP, add_heads, jnp.zeros((total, D), jnp.float32)).astype(jnp.bfloat16)
    normed = layer_normed(moe_rows, moe_gain)
    devices = MOE_TOKENS // MOE_DEV
    chosen = routes.reshape(devices, MOE_DEV * TOP).astype(jnp.int32)
    onehot = (chosen[..., None] == jnp.arange(EXPERTS, dtype=jnp.int32)[None, None, :]).astype(jnp.int32)
    earlier_count = jnp.cumsum(onehot, 1) - onehot
    slot_index = lax.optimization_barrier(jnp.sum(earlier_count * onehot, -1)).astype(jnp.int32)
    device_index = jnp.arange(devices, dtype=jnp.int32)[:, None]
    position = ((chosen * devices + device_index) * CAP + slot_index).reshape(-1).astype(jnp.int32)
    token_of = (jnp.arange(MOE_TOKENS * TOP, dtype=jnp.int32) // TOP).astype(jnp.int32)
    buffer = jnp.zeros((EXPERTS * devices * CAP, D), jnp.bfloat16).at[position].set(normed[token_of])
    buffer = buffer.reshape(EXPERTS, devices * CAP, D)
    results = lax.map(one_expert, (buffer, gate_weight, up_weight, down_weight))
    picked = results.reshape(EXPERTS * devices * CAP, D)[position].astype(jnp.float32)
    picked = picked.reshape(MOE_TOKENS, TOP, D)
    moe_out = lax.optimization_barrier(jnp.sum(picked * route_weight[:, :, None], 1)).astype(jnp.bfloat16)
    return (mixer_out, moe_out)
```

```python
import functools

import jax
import jax.numpy as jnp
from jax import lax
from jax.experimental import pallas as pl
from jax.experimental.pallas import tpu as pltpu
from jax.sharding import PartitionSpec as P


HEADS = 16
KV_HEADS = 2
HEAD_DIM = 64
WINDOW = 128
TOP = 2
CORES = 2


big_negative = -1e30
norm_eps = 1e-05
BF = jnp.bfloat16
F32 = jnp.float32
VMEM = pl.BlockSpec(memory_space=pltpu.VMEM)
SMEM = pl.BlockSpec(memory_space=pltpu.SMEM)
HBM = pl.BlockSpec(memory_space=pltpu.HBM)


def swapped(value, axis, mask):
    count = lax.axis_size(axis)
    return lax.ppermute(value, axis, [(i, i ^ mask) for i in range(count)])


def small(mib):
    return pltpu.CompilerParams(vmem_limit_bytes=mib << 20)


def fetch(sources, targets, sems):
    copies = [pltpu.make_async_copy(s, t, sems.at[i]) for i, (s, t) in enumerate(zip(sources, targets))]
    for copy in copies:
        copy.start()
    return copies


def cost(flops, moved):
    return pl.CostEstimate(flops=int(flops), bytes_accessed=int(moved), transcendentals=0)


def nt(a, b):
    return lax.dot_general(a, b, (((1,), (1,)), ((), ())), preferred_element_type=F32)


def relative(i, groups_z):
    far, core, k = i // (2 * groups_z), (i // groups_z) % 2, i % groups_z
    return far * (2 * groups_z) + 2 * k + core


def attend_kernel(where_ref, sink_ref, q_hbm, k_hbm, v_hbm, early_ref, *refs):
    out_refs, (q_ref, k_ref, v_ref, sems) = refs[:4], refs[4:]
    for copy in fetch((q_hbm, k_hbm, v_hbm), (q_ref, k_ref, v_ref), sems):
        copy.wait()
    blocks = q_ref.shape[0] // WINDOW
    heads_here = q_ref.shape[1] // HEAD_DIM
    groups_z = blocks // 4
    key_head = where_ref[1]
    width = KV_HEADS * HEAD_DIM

    def own(values):
        parts = [values[:, h * HEAD_DIM : (h + 1) * HEAD_DIM] for h in range(KV_HEADS)]
        picked = parts[0]
        for h in range(1, KV_HEADS):
            picked = jnp.where(key_head == h, parts[h], picked)
        return picked

    row = lax.broadcasted_iota(jnp.int32, (WINDOW, WINDOW), 0)
    col = lax.broadcasted_iota(jnp.int32, (WINDOW, WINDOW), 1)
    cur_ok = col <= row
    for i in range(blocks):
        block = where_ref[0] ^ relative(i, groups_z)
        first = block == 0
        no_past = jnp.logical_and(first, where_ref[2] == 0)
        here = pl.ds(pl.multiple_of(block * WINDOW, WINDOW), WINDOW)
        past = pl.ds(pl.multiple_of(jnp.maximum(block - 1, 0) * WINDOW, WINDOW), WINDOW)
        k_cur, v_cur = own(k_ref[here, :]), own(v_ref[here, :])
        k_past = own(jnp.where(first, early_ref[:, :width], k_ref[past, :]))
        v_past = own(jnp.where(first, early_ref[:, width:], v_ref[past, :]))
        past_ok = jnp.logical_and(col > row, jnp.logical_not(no_past))
        out_ref, place = out_refs[i // groups_z], (i % groups_z) * WINDOW
        for h in range(heads_here):
            cols = slice(h * HEAD_DIM, (h + 1) * HEAD_DIM)
            q = q_ref[here, cols]
            sink = sink_ref[h]
            s_past = jnp.where(past_ok, nt(q, k_past) * HEAD_DIM ** (-0.5), big_negative)
            s_cur = jnp.where(cur_ok, nt(q, k_cur) * HEAD_DIM ** (-0.5), big_negative)
            top = jnp.maximum(jnp.max(jnp.maximum(s_past, s_cur), -1, keepdims=True), sink)
            e_past = jnp.where(past_ok, jnp.exp(s_past - top), 0.0)
            e_cur = jnp.where(cur_ok, jnp.exp(s_cur - top), 0.0)
            total = jnp.sum(e_past + e_cur, -1, keepdims=True) + jnp.exp(sink - top)
            scale = 1.0 / total
            mixed = jnp.dot((e_past * scale).astype(BF), v_past, preferred_element_type=F32)
            mixed += jnp.dot((e_cur * scale).astype(BF), v_cur, preferred_element_type=F32)
            out_ref[place : place + WINDOW, cols] = mixed.astype(BF)


def attend(queries, key_rows, value_rows, sink_logits, earlier):
    total, cols = queries.shape
    assert total // lax.axis_size("tp") == WINDOW
    tp = lax.axis_index("tp")
    key_head = tp * sink_logits.shape[0] // (HEADS // KV_HEADS)
    place = jnp.stack([tp, key_head, lax.axis_index("ep")]).astype(jnp.int32)
    return pl.pallas_call(
        attend_kernel,
        in_specs=[SMEM, SMEM] + [HBM] * 3 + [VMEM],
        out_specs=[VMEM] * 4,
        out_shape=[jax.ShapeDtypeStruct((total // 4, cols), BF)] * 4,
        scratch_shapes=[pltpu.VMEM(a.shape, BF) for a in (queries, key_rows, value_rows)]
        + [pltpu.SemaphoreType.DMA((3,))],
        cost_estimate=cost(4e9, 2e6),
        compiler_params=small(8),
        name="attend",
    )(place, sink_logits, queries, key_rows, value_rows, earlier)


def project_kernel(count, *refs):
    parts, mats, outs = refs[:count], refs[count : 2 * count], refs[2 * count :]
    rows = outs[0].shape[0]
    width = mats[0].shape[1]
    tile = min(512, width)
    for n in range(0, width, tile):
        total = None
        for part, mat in zip(parts, mats):
            term = jnp.dot(part[...], mat[:, n : n + tile], preferred_element_type=F32)
            total = term if total is None else total + term
        for i, out in enumerate(outs):
            out[:, n : n + tile] = total[i * rows : (i + 1) * rows].astype(out.dtype)


def project(parts, mats):
    rows = parts[0].shape[0]
    width = mats[0].shape[1]
    groups = rows // WINDOW
    out = [jax.ShapeDtypeStruct((WINDOW, width), F32 if i == 0 else BF) for i in range(groups)]
    return pl.pallas_call(
        functools.partial(project_kernel, len(parts)),
        in_specs=[VMEM] * (2 * len(parts)),
        out_specs=[VMEM] * groups,
        out_shape=out,
        cost_estimate=cost(2e9, 4e6),
        compiler_params=small(12),
        name="project",
    )(*parts, *mats)


def norm_kernel(experts, *refs):
    sources, (out_ref, last_ref), targets, sems = refs[:6], refs[6:8], refs[8:14], refs[14]
    x_ref, gain_ref, routes_ref, weight_ref, k_ref, v_ref = targets
    end = pl.ds(sources[4].shape[0] - WINDOW, WINDOW)
    copies = fetch(sources[:4] + (sources[4].at[end], sources[5].at[end]), targets, sems)
    for copy in copies:
        copy.wait()
    width = x_ref.shape[1]
    values = x_ref[...].astype(F32)
    center = values - jnp.mean(values, -1, keepdims=True)
    spread = jnp.mean(center * center, -1, keepdims=True)
    out_ref[:, :width] = (center * lax.rsqrt(spread + norm_eps) * gain_ref[...]).astype(BF)
    lane = lax.broadcasted_iota(jnp.int32, (128, x_ref.shape[0]), 0)
    expert = jnp.where(lane < experts, lane, lane - experts)
    weight = jnp.zeros(lane.shape, F32)
    for k in range(TOP):
        weight += jnp.where(routes_ref[k : k + 1, :] == expert, weight_ref[k : k + 1, :], 0.0)
    high = weight.astype(BF).astype(F32)
    table = jnp.where(lane < experts, high, jnp.where(lane < 2 * experts, weight - high, 0.0))
    out_ref[:, width:] = table.T.astype(BF)
    last_ref[:, : k_ref.shape[1]] = k_ref[...]
    last_ref[:, k_ref.shape[1] :] = v_ref[...]


def normed_rows(moe_rows, moe_gain, routes, route_weight, experts, key_rows, value_rows):
    rows, width = moe_rows.shape
    cols = key_rows.shape[1]
    args = (moe_rows, moe_gain[None, :], routes.T, route_weight.T, key_rows, value_rows)
    shapes = [a.shape for a in args[:4]] + [(WINDOW, cols)] * 2
    return pl.pallas_call(
        functools.partial(norm_kernel, experts),
        in_specs=[HBM] * 6,
        out_specs=[VMEM] * 2,
        out_shape=[
            jax.ShapeDtypeStruct((rows, width + 128), BF),
            jax.ShapeDtypeStruct((WINDOW, 2 * cols), BF),
        ],
        scratch_shapes=[pltpu.VMEM(shape, a.dtype) for shape, a in zip(shapes, args)]
        + [pltpu.SemaphoreType.DMA((6,))],
        cost_estimate=cost(1e7, 3e5),
        compiler_params=small(8),
        name="normed",
    )(*args)


def slots_of(experts, capacity, blocks, width):
    rows = blocks[0].shape[0]
    tokens = rows * len(blocks)
    table = jnp.concatenate([b[:, width:] for b in blocks], 0).astype(F32).T
    flags = (table > 0).astype(BF)
    source = lax.broadcasted_iota(jnp.int32, (tokens, tokens), 0)
    target = lax.broadcasted_iota(jnp.int32, (tokens, tokens), 1)
    ahead = jnp.logical_and(source < target, source // rows == target // rows).astype(BF)
    position = jnp.dot(flags, ahead, preferred_element_type=F32)
    lane = lax.broadcasted_iota(jnp.int32, (128, tokens), 0)
    base = (lax.broadcasted_iota(jnp.int32, (1, tokens), 1) // rows) * capacity

    def of(expert):
        high = jnp.sum(jnp.where(lane == expert, table, 0.0), 0, keepdims=True)
        low = jnp.sum(jnp.where(lane == expert + experts, table, 0.0), 0, keepdims=True)
        place = jnp.sum(jnp.where(lane == expert, position, 0.0), 0, keepdims=True)
        return jnp.where(high > 0, base + place.astype(jnp.int32), -1), high, low

    return of


def pick_kernel(experts, capacity, ep_ref, *refs):
    lines = len(refs) - experts
    blocks, picked = refs[:lines], refs[lines:]
    slots, width = picked[0].shape
    of = slots_of(experts, capacity, blocks, width)
    slot_id = lax.broadcasted_iota(jnp.int32, (slots, blocks[0].shape[0] * lines), 0)
    values = jnp.concatenate([b[:, :width] for b in blocks], 0)
    for k in range(experts):
        hit = (slot_id == of(ep_ref[0] ^ k)[0]).astype(BF)
        picked[k][...] = jnp.dot(hit, values, preferred_element_type=F32).astype(BF)


def maps_kernel(experts, capacity, ep_ref, *refs):
    lines = len(refs) - 1
    blocks, maps_ref = refs[:lines], refs[lines]
    slots = capacity * lines
    of = slots_of(experts, capacity, blocks, 0)
    slot_id = lax.broadcasted_iota(jnp.int32, (slots, blocks[0].shape[0] * lines), 0)
    for k in range(experts):
        slot, high, low = of(ep_ref[0] ^ k)
        hit = slot_id == slot
        for j, part in enumerate((high, low)):
            maps_ref[2 * k + j] = jnp.where(hit, part, 0.0).T.astype(BF)


def pick(blocks, experts, capacity):
    _, width = blocks[0].shape
    width -= 128
    slots = capacity * len(blocks)
    ep = lax.axis_index("ep").astype(jnp.int32)[None]
    return pl.pallas_call(
        functools.partial(pick_kernel, experts, capacity),
        in_specs=[SMEM] + [VMEM] * len(blocks),
        out_specs=[VMEM] * experts,
        out_shape=[jax.ShapeDtypeStruct((slots, width), BF)] * experts,
        cost_estimate=cost(2e8, 2e6),
        compiler_params=small(12),
        name="pick",
    )(ep, *blocks)


def weight_maps(blocks, experts, capacity):
    rows, width = blocks[0].shape
    slots, tokens = capacity * len(blocks), rows * len(blocks)
    ep = lax.axis_index("ep").astype(jnp.int32)[None]
    tail = pl.BlockSpec((rows, 128), lambda i: (0, width // 128 - 1))
    return pl.pallas_call(
        functools.partial(maps_kernel, experts, capacity),
        grid=(1,),
        in_specs=[SMEM] + [tail] * len(blocks),
        out_specs=pl.BlockSpec((2 * experts, tokens, slots), lambda i: (0, 0, 0)),
        out_shape=jax.ShapeDtypeStruct((2 * experts, tokens, slots), BF),
        cost_estimate=cost(2e7, 1e6),
        compiler_params=small(12),
        name="maps",
    )(ep, *blocks)


def expert_kernel(count, *refs):
    rows_refs = refs[:count]
    own_mats, other_mats = refs[count : count + 3], refs[count + 3 : count + 6]
    outs = refs[count + 6 : 2 * count + 6]
    all_rows, hidden, sems = refs[2 * count + 6 : 2 * count + 9]
    held = refs[2 * count + 9 :]
    copies = fetch(other_mats, held, sems)
    gates, ups, downs = zip(own_mats, held)
    slots, width = rows_refs[0].shape
    units = gates[0].shape[1]
    for i in range(count):
        all_rows[i * slots : (i + 1) * slots, :] = rows_refs[i][...]
    tile = 256
    for j in range(2):
        if j == 1:
            copies[0].wait()
            copies[1].wait()
        for n in range(0, units, tile):
            cols = slice(n, min(n + tile, units))
            g = jnp.dot(all_rows[...], gates[j][:, cols], preferred_element_type=F32)
            u = jnp.dot(all_rows[...], ups[j][:, cols], preferred_element_type=F32)
            hidden[j, :, cols] = (g / (1.0 + jnp.exp(-g)) * u).astype(BF)
    copies[2].wait()
    for n in range(0, width, tile):
        cols = slice(n, n + tile)
        total = jnp.dot(hidden[0], downs[0][:, cols], preferred_element_type=F32)
        total += jnp.dot(hidden[1], downs[1][:, cols], preferred_element_type=F32)
        for i in range(count):
            outs[i][:, cols] = total[i * slots : (i + 1) * slots].astype(BF)


def expert(row_sets, own_mats, other_mats):
    count = len(row_sets)
    slots, width = row_sets[0].shape
    units = own_mats[0].shape[1]
    total = count * slots
    return pl.pallas_call(
        functools.partial(expert_kernel, count),
        in_specs=[VMEM] * (count + 3) + [HBM] * 3,
        out_specs=[VMEM] * count,
        out_shape=[jax.ShapeDtypeStruct((slots, width), BF)] * count,
        scratch_shapes=[
            pltpu.VMEM((total, width), BF),
            pltpu.VMEM((2, total, units), BF),
            pltpu.SemaphoreType.DMA((3,)),
        ]
        + [pltpu.VMEM(m.shape, BF) for m in other_mats],
        cost_estimate=cost(12 * total * width * units, 12 * width * units),
        compiler_params=small(22),
        name="expert",
    )(*row_sets, *own_mats, *other_mats)


def combine_kernel(experts, maps_ref, *refs):
    results, outs = refs[:experts], refs[experts:]
    rows, width = outs[0].shape
    tile = min(512, width)
    for n in range(0, width, tile):
        cols = slice(n, n + tile)
        total = None
        for k in range(experts):
            for j in range(2):
                term = jnp.dot(maps_ref[2 * k + j], results[k][:, cols], preferred_element_type=F32)
                total = term if total is None else total + term
        for i, out in enumerate(outs):
            out[:, cols] = total[i * rows : (i + 1) * rows].astype(out.dtype)


def combine(maps, results, lines):
    experts = len(results)
    width = results[0].shape[1]
    rows = maps.shape[1] // lines
    out = [jax.ShapeDtypeStruct((rows, width), F32 if i == 0 else BF) for i in range(lines)]
    return pl.pallas_call(
        functools.partial(combine_kernel, experts),
        in_specs=[VMEM] * (1 + experts),
        out_specs=[VMEM] * lines,
        out_shape=out,
        cost_estimate=cost(5e8, 3e6),
        compiler_params=small(12),
        name="combine",
    )(maps, *results)


def body(
    queries,
    key_rows,
    value_rows,
    sink_logits,
    out_weight,
    moe_rows,
    moe_gain,
    routes,
    route_weight,
    gate_weight,
    up_weight,
    down_weight,
):
    tp, ep = lax.axis_size("tp"), lax.axis_size("ep")
    lines, far = tp // CORES, tp // 2
    experts_all = gate_weight.shape[0] * ep
    capacity = 3 * moe_rows.shape[0] * TOP // (2 * experts_all)

    own_mats = (gate_weight[0], up_weight[0], down_weight[0])
    other_mats = [swapped(m, "tp", 1) for m in own_mats]

    own, last = normed_rows(
        moe_rows, moe_gain, routes, route_weight, experts_all, key_rows, value_rows
    )
    blocks = [own] + [swapped(own, "tp", CORES * k) for k in range(1, lines)]
    earlier = lax.ppermute(last, "ep", [(i, i + 1) for i in range(ep - 1)])

    picked = pick(blocks, experts_all, capacity)
    arrived = [picked[0]] + [swapped(picked[k], "ep", k) for k in range(1, ep)]
    maps = weight_maps(blocks, experts_all, capacity)

    pieces = attend(queries, key_rows, value_rows, sink_logits, earlier)
    parts = [pieces[0]] + [
        swapped(pieces[i], "tp", mask)
        for i, mask in ((1, 1), (2, far), (3, far + 1))
    ]
    far_weight = swapped(out_weight, "tp", far)
    mats = [out_weight, swapped(out_weight, "tp", 1), far_weight, swapped(far_weight, "tp", 1)]
    shares = project(parts, mats)
    mixer = shares[0]
    for k in range(1, far // CORES):
        mixer += swapped(shares[k], "tp", CORES * k).astype(F32)

    order = list(range(1, ep)) + [0]
    results = [None] * ep
    for group in (order[: ep // 2], order[ep // 2 :]):
        done = expert([arrived[k] for k in group], own_mats, other_mats)
        for k, value in zip(group, done):
            results[k] = value
    returned = [results[0]] + [swapped(results[k], "ep", k) for k in range(1, ep)]

    sums = combine(maps, returned, lines)
    moe = sums[0]
    for k in range(1, lines):
        moe += swapped(sums[k], "tp", CORES * k).astype(F32)
    return (mixer.astype(BF), moe.astype(BF))


def solution(mesh):
    in_specs = (
        P("ep", "tp"),
        P("ep", None),
        P("ep", None),
        P("tp"),
        P("tp", None),
        P(("ep", "tp"), None),
        P(),
        P(("ep", "tp"), None),
        P(("ep", "tp"), None),
        P("ep", None, "tp"),
        P("ep", None, "tp"),
        P("ep", "tp", None),
    )
    out_specs = (P(("ep", "tp"), None), P(("ep", "tp"), None))
    return jax.shard_map(body, mesh=mesh, in_specs=in_specs, out_specs=out_specs, check_vma=False)
```

```python
import functools

import jax
import jax.numpy as jnp
from jax import lax
from jax.experimental import pallas as pl
from jax.experimental.pallas import tpu as pltpu
from jax.sharding import PartitionSpec as P


HEADS = 16
KV_HEADS = 2
HEAD_DIM = 64
WINDOW = 128
TOP = 2
CORES = 2


big_negative = -1e30
norm_eps = 1e-05
BF = jnp.bfloat16
F32 = jnp.float32
VMEM = pl.BlockSpec(memory_space=pltpu.VMEM)
SMEM = pl.BlockSpec(memory_space=pltpu.SMEM)
HBM = pl.BlockSpec(memory_space=pltpu.HBM)


def swapped(value, axis, mask):
    count = lax.axis_size(axis)
    return lax.ppermute(value, axis, [(i, i ^ mask) for i in range(count)])


def small(mib):
    return pltpu.CompilerParams(vmem_limit_bytes=mib << 20)


def fetch(sources, targets, sems):
    copies = [pltpu.make_async_copy(s, t, sems.at[i]) for i, (s, t) in enumerate(zip(sources, targets))]
    for copy in copies:
        copy.start()
    return copies


def far_away(value):
    return pltpu.with_memory_space_constraint(value, pltpu.HBM)


def cost(flops, moved):
    return pl.CostEstimate(flops=int(flops), bytes_accessed=int(moved), transcendentals=0)


def nt(a, b):
    return lax.dot_general(a, b, (((1,), (1,)), ((), ())), preferred_element_type=F32)


def relative(i, groups_z):
    far, core, k = i // (2 * groups_z), (i // groups_z) % 2, i % groups_z
    return 2 * CORES * k + CORES * far + core


def attend_kernel(where_ref, sink_ref, q_hbm, k_hbm, v_hbm, early_ref, *refs):
    out_refs, (q_ref, kv_ref, k_ext, v_ext, sems) = refs[:3], refs[3:]
    copies = fetch((q_hbm, k_hbm, v_hbm), (q_ref, kv_ref.at[0], kv_ref.at[1]), sems)
    blocks = q_ref.shape[0] // WINDOW
    cols = q_ref.shape[1]
    heads_here = cols // HEAD_DIM
    groups_z = blocks // 4
    key_head = where_ref[1]
    width = KV_HEADS * HEAD_DIM

    def own(values):
        parts = [values[:, h * HEAD_DIM : (h + 1) * HEAD_DIM] for h in range(KV_HEADS)]
        picked = parts[0]
        for h in range(1, KV_HEADS):
            picked = jnp.where(key_head == h, parts[h], picked)
        return picked

    k_ext[...] = jnp.zeros_like(k_ext)
    v_ext[:, :, :cols] = jnp.zeros((heads_here, v_ext.shape[1], cols), BF)
    v_ext[:, :, cols:] = jnp.ones((heads_here, v_ext.shape[1], cols), BF)
    early_k, early_v = own(early_ref[:, :width]), own(early_ref[:, width:])
    for h in range(heads_here):
        place = slice(h * HEAD_DIM, (h + 1) * HEAD_DIM)
        k_ext[h, :WINDOW, place] = early_k
        v_ext[h, :WINDOW, place] = early_v
    for copy in copies:
        copy.wait()
    own_k, own_v = own(kv_ref[0]), own(kv_ref[1])
    for h in range(heads_here):
        place = slice(h * HEAD_DIM, (h + 1) * HEAD_DIM)
        k_ext[h, WINDOW:, place] = own_k
        v_ext[h, WINDOW:, place] = own_v

    row = lax.broadcasted_iota(jnp.int32, (WINDOW, 2 * WINDOW), 0)
    col = lax.broadcasted_iota(jnp.int32, (WINDOW, 2 * WINDOW), 1)
    near = jnp.logical_and(col > row, col <= row + WINDOW)
    for i in range(blocks):
        block = where_ref[0] ^ relative(i, groups_z)
        no_past = jnp.logical_and(block == 0, where_ref[2] == 0)
        allowed = jnp.logical_and(near, col >= jnp.where(no_past, WINDOW, 0))
        start = pl.multiple_of(block * WINDOW, WINDOW)
        q = q_ref[pl.ds(start, WINDOW), :] * HEAD_DIM ** (-0.5)
        mixed = None
        for h in range(heads_here):
            sink = sink_ref[h]
            window = pl.ds(start, 2 * WINDOW)
            scores = jnp.where(allowed, nt(q, k_ext[h, window, :]), big_negative)
            top = jnp.maximum(jnp.max(scores, -1, keepdims=True), sink)
            powers = jnp.exp(scores - top).astype(BF)
            both = jnp.dot(powers, v_ext[h, window, :], preferred_element_type=F32)
            part = both[:, :cols] / (both[:, cols:] + jnp.exp(sink - top))
            mixed = part if mixed is None else mixed + part
        group, place = i // groups_z, i % groups_z
        if group >= 2:
            place += (group - 2) * groups_z
        out_refs[min(group, 2)][place * WINDOW : (place + 1) * WINDOW, :] = mixed.astype(BF)


def attend(queries, key_rows, value_rows, sink_logits, earlier):
    total, cols = queries.shape
    assert total // lax.axis_size("tp") == WINDOW
    tp = lax.axis_index("tp")
    key_head = tp * sink_logits.shape[0] // (HEADS // KV_HEADS)
    place = jnp.stack([tp, key_head, lax.axis_index("ep")]).astype(jnp.int32)
    return pl.pallas_call(
        attend_kernel,
        in_specs=[SMEM, SMEM] + [HBM] * 3 + [VMEM],
        out_specs=[VMEM] * 3,
        out_shape=[jax.ShapeDtypeStruct((total // n, cols), BF) for n in (4, 4, 2)],
        scratch_shapes=[
            pltpu.VMEM(queries.shape, BF),
            pltpu.VMEM((2,) + key_rows.shape, BF),
            pltpu.VMEM((cols // HEAD_DIM, total + WINDOW, cols), BF),
            pltpu.VMEM((cols // HEAD_DIM, total + WINDOW, 2 * cols), BF),
            pltpu.SemaphoreType.DMA((3,)),
        ],
        cost_estimate=cost(4e9, 2e6),
        compiler_params=small(8),
        name="attend",
    )(place, sink_logits, *map(far_away, (queries, key_rows, value_rows)), earlier)


def project_kernel(*refs):
    parts, mats, outs = refs[:4], refs[4:8], refs[8:]
    rows = outs[0].shape[0]
    here = parts[0].shape[0]
    width = mats[0].shape[1]
    tile = min(512, width)
    for n in range(0, width, tile):
        total = None
        for i, (part, mat) in enumerate(zip(parts, mats)):
            left = part[here:, :] if i == 3 else part[:here, :]
            term = jnp.dot(left, mat[:, n : n + tile], preferred_element_type=F32)
            total = term if total is None else total + term
        for i, out in enumerate(outs):
            out[:, n : n + tile] = total[i * rows : (i + 1) * rows].astype(out.dtype)


def project(parts, mats):
    rows = parts[0].shape[0]
    width = mats[0].shape[1]
    groups = rows // WINDOW
    out = [jax.ShapeDtypeStruct((WINDOW, width), F32 if i == 0 else BF) for i in range(groups)]
    return pl.pallas_call(
        project_kernel,
        in_specs=[VMEM] * 8,
        out_specs=[VMEM] * groups,
        out_shape=out,
        cost_estimate=cost(2e9, 4e6),
        compiler_params=small(12),
        name="project",
    )(*parts, *mats)


def norm_kernel(experts, *refs):
    sources, (out_ref, last_ref), targets, sems = refs[:6], refs[6:8], refs[8:14], refs[14]
    x_ref, gain_ref, routes_ref, weight_ref, k_ref, v_ref = targets
    end = pl.ds(sources[4].shape[0] - WINDOW, WINDOW)
    copies = fetch(sources[:4] + (sources[4].at[end], sources[5].at[end]), targets, sems)
    for copy in copies:
        copy.wait()
    width = x_ref.shape[1]
    values = x_ref[...].astype(F32)
    center = values - jnp.mean(values, -1, keepdims=True)
    spread = jnp.mean(center * center, -1, keepdims=True)
    out_ref[:, :width] = (center * lax.rsqrt(spread + norm_eps) * gain_ref[...]).astype(BF)
    lane = lax.broadcasted_iota(jnp.int32, (128, x_ref.shape[0]), 0)
    expert = jnp.where(lane < experts, lane, lane - experts)
    weight = jnp.zeros(lane.shape, F32)
    for k in range(TOP):
        weight += jnp.where(routes_ref[k : k + 1, :] == expert, weight_ref[k : k + 1, :], 0.0)
    high = weight.astype(BF).astype(F32)
    table = jnp.where(lane < experts, high, jnp.where(lane < 2 * experts, weight - high, 0.0))
    out_ref[:, width:] = table.T.astype(BF)
    last_ref[:, : k_ref.shape[1]] = k_ref[...]
    last_ref[:, k_ref.shape[1] :] = v_ref[...]


def normed_rows(moe_rows, moe_gain, routes, route_weight, experts, key_rows, value_rows):
    rows, width = moe_rows.shape
    cols = key_rows.shape[1]
    args = (moe_rows, moe_gain[None, :], routes.T, route_weight.T, key_rows, value_rows)
    shapes = [a.shape for a in args[:4]] + [(WINDOW, cols)] * 2
    return pl.pallas_call(
        functools.partial(norm_kernel, experts),
        in_specs=[HBM] * 6,
        out_specs=[VMEM] * 2,
        out_shape=[
            jax.ShapeDtypeStruct((rows, width + 128), BF),
            jax.ShapeDtypeStruct((WINDOW, 2 * cols), BF),
        ],
        scratch_shapes=[pltpu.VMEM(shape, a.dtype) for shape, a in zip(shapes, args)]
        + [pltpu.SemaphoreType.DMA((6,))],
        cost_estimate=cost(1e7, 3e5),
        compiler_params=small(8),
        name="normed",
    )(*map(far_away, args))


def slots_of(experts, capacity, blocks, width):
    rows = blocks[0].shape[0]
    tokens = rows * len(blocks)
    table = jnp.concatenate([b[:, width:] for b in blocks], 0).astype(F32).T
    flags = (table > 0).astype(BF)
    source = lax.broadcasted_iota(jnp.int32, (tokens, tokens), 0)
    target = lax.broadcasted_iota(jnp.int32, (tokens, tokens), 1)
    ahead = jnp.logical_and(source < target, source // rows == target // rows).astype(BF)
    position = jnp.dot(flags, ahead, preferred_element_type=F32)
    lane = lax.broadcasted_iota(jnp.int32, (128, tokens), 0)
    base = (lax.broadcasted_iota(jnp.int32, (1, tokens), 1) // rows) * capacity

    def of(expert):
        high = jnp.sum(jnp.where(lane == expert, table, 0.0), 0, keepdims=True)
        low = jnp.sum(jnp.where(lane == expert + experts, table, 0.0), 0, keepdims=True)
        place = jnp.sum(jnp.where(lane == expert, position, 0.0), 0, keepdims=True)
        return jnp.where(high > 0, base + place.astype(jnp.int32), -1), high, low

    return of


def pick_kernel(experts, capacity, ep_ref, *refs):
    lines = len(refs) - experts
    blocks, picked = refs[:lines], refs[lines:]
    slots, width = picked[0].shape
    of = slots_of(experts, capacity, blocks, width)
    slot_id = lax.broadcasted_iota(jnp.int32, (slots, blocks[0].shape[0] * lines), 0)
    values = jnp.concatenate([b[:, :width] for b in blocks], 0)
    for k in range(experts):
        hit = (slot_id == of(ep_ref[0] ^ k)[0]).astype(BF)
        picked[k][...] = jnp.dot(hit, values, preferred_element_type=F32).astype(BF)


def maps_kernel(experts, capacity, ep_ref, *refs):
    lines = len(refs) - 1
    blocks, maps_ref = refs[:lines], refs[lines]
    slots = capacity * lines
    of = slots_of(experts, capacity, blocks, 0)
    slot_id = lax.broadcasted_iota(jnp.int32, (slots, blocks[0].shape[0] * lines), 0)
    for k in range(experts):
        slot, high, low = of(ep_ref[0] ^ k)
        hit = slot_id == slot
        for j, part in enumerate((high, low)):
            maps_ref[2 * k + j] = jnp.where(hit, part, 0.0).T.astype(BF)


def pick(blocks, experts, capacity):
    _, width = blocks[0].shape
    width -= 128
    slots = capacity * len(blocks)
    ep = lax.axis_index("ep").astype(jnp.int32)[None]
    return pl.pallas_call(
        functools.partial(pick_kernel, experts, capacity),
        in_specs=[SMEM] + [VMEM] * len(blocks),
        out_specs=[VMEM] * experts,
        out_shape=[jax.ShapeDtypeStruct((slots, width), BF)] * experts,
        cost_estimate=cost(2e8, 2e6),
        compiler_params=small(12),
        name="pick",
    )(ep, *blocks)


def weight_maps(blocks, experts, capacity):
    rows, width = blocks[0].shape
    slots, tokens = capacity * len(blocks), rows * len(blocks)
    ep = lax.axis_index("ep").astype(jnp.int32)[None]
    tail = pl.BlockSpec((rows, 128), lambda i: (0, width // 128 - 1))
    return pl.pallas_call(
        functools.partial(maps_kernel, experts, capacity),
        grid=(1,),
        in_specs=[SMEM] + [tail] * len(blocks),
        out_specs=pl.BlockSpec((2 * experts, tokens, slots), lambda i: (0, 0, 0)),
        out_shape=jax.ShapeDtypeStruct((2 * experts, tokens, slots), BF),
        cost_estimate=cost(2e7, 1e6),
        compiler_params=small(12),
        name="maps",
    )(ep, *blocks)


def expert_kernel(count, fetching, *refs):
    rows_refs, mats, refs = refs[:count], (refs[count : count + 3], refs[count + 3 : count + 6]), refs[count + 6 :]
    outs, refs = refs[:count], refs[count:]
    copies = [None] * 3
    if fetching:
        held, refs = refs[:3], refs[3:]
        copies = fetch(mats[1], held, refs[3])
        mats = mats[0], held
    all_rows, hidden, total = refs[:3]
    slots, width = rows_refs[0].shape
    units = mats[0][0].shape[1]
    for i in range(count):
        all_rows[i * slots : (i + 1) * slots, :] = rows_refs[i][...]
    tile = 256
    for j, (gate, up, down) in enumerate(mats):
        if fetching and j == 1:
            copies[0].wait()
            copies[1].wait()
        for n in range(0, units, tile):
            cols = slice(n, min(n + tile, units))
            g = jnp.dot(all_rows[...], gate[:, cols], preferred_element_type=F32)
            u = jnp.dot(all_rows[...], up[:, cols], preferred_element_type=F32)
            hidden[j, :, cols] = (g / (1.0 + jnp.exp(-g)) * u).astype(BF)
        if fetching and j == 0:
            for n in range(0, width, tile):
                cols = slice(n, n + tile)
                total[:, cols] = jnp.dot(hidden[0], down[:, cols], preferred_element_type=F32)
    if fetching:
        copies[2].wait()
    for n in range(0, width, tile):
        cols = slice(n, n + tile)
        if fetching:
            term = total[:, cols]
        else:
            term = jnp.dot(hidden[0], mats[0][2][:, cols], preferred_element_type=F32)
        term += jnp.dot(hidden[1], mats[1][2][:, cols], preferred_element_type=F32)
        for i in range(count):
            outs[i][:, cols] = term[i * slots : (i + 1) * slots].astype(BF)


def expert(row_sets, own_mats, other_mats, fetching):
    count = len(row_sets)
    slots, width = row_sets[0].shape
    units = own_mats[0].shape[1]
    total = count * slots
    out = [jax.ShapeDtypeStruct((slots, width), BF)] * count
    scratch = [
        pltpu.VMEM((total, width), BF),
        pltpu.VMEM((2, total, units), BF),
        pltpu.VMEM((total, width), F32),
    ]
    if fetching:
        out += [jax.ShapeDtypeStruct(m.shape, BF) for m in other_mats]
        scratch.append(pltpu.SemaphoreType.DMA((3,)))
        other_mats = list(map(far_away, other_mats))
    result = pl.pallas_call(
        functools.partial(expert_kernel, count, fetching),
        in_specs=[VMEM] * (count + 3) + [HBM if fetching else VMEM] * 3,
        out_specs=[VMEM] * len(out),
        out_shape=out,
        scratch_shapes=scratch,
        cost_estimate=cost(12 * total * width * units, 12 * width * units),
        compiler_params=small(16),
        name="expert",
    )(*row_sets, *own_mats, *other_mats)
    return result[:count], result[count:] if fetching else other_mats


def combine_kernel(experts, maps_ref, *refs):
    results, outs = refs[:experts], refs[experts:]
    rows, width = outs[0].shape
    tile = min(512, width)
    for n in range(0, width, tile):
        cols = slice(n, n + tile)
        total = None
        for k in range(experts):
            for j in range(2):
                term = jnp.dot(maps_ref[2 * k + j], results[k][:, cols], preferred_element_type=F32)
                total = term if total is None else total + term
        for i, out in enumerate(outs):
            out[:, cols] = total[i * rows : (i + 1) * rows].astype(out.dtype)


def combine(maps, results, lines, kept):
    experts = len(results)
    width = results[0].shape[1]
    rows = maps.shape[1] // lines
    out = [jax.ShapeDtypeStruct((rows, width), F32 if i == 0 and kept else BF) for i in range(lines)]
    return pl.pallas_call(
        functools.partial(combine_kernel, experts),
        in_specs=[VMEM] * (1 + experts),
        out_specs=[VMEM] * lines,
        out_shape=out,
        cost_estimate=cost(5e8, 3e6),
        compiler_params=small(12),
        name="combine",
    )(maps, *results)


def body(
    queries,
    key_rows,
    value_rows,
    sink_logits,
    out_weight,
    moe_rows,
    moe_gain,
    routes,
    route_weight,
    gate_weight,
    up_weight,
    down_weight,
):
    tp, ep = lax.axis_size("tp"), lax.axis_size("ep")
    lines, far = tp // CORES, CORES
    experts_all = gate_weight.shape[0] * ep
    capacity = 3 * moe_rows.shape[0] * TOP // (2 * experts_all)

    own, last = normed_rows(
        moe_rows, moe_gain, routes, route_weight, experts_all, key_rows, value_rows
    )
    blocks = [own] + [swapped(own, "tp", CORES * k) for k in range(1, lines)]
    earlier = lax.ppermute(last, "ep", [(i, i + 1) for i in range(ep - 1)])
    own_mats = (gate_weight[0], up_weight[0], down_weight[0])
    other_mats = [swapped(m, "tp", 1) for m in own_mats]

    pieces = attend(queries, key_rows, value_rows, sink_logits, earlier)
    far_heads = swapped(pieces[2], "tp", far)
    parts = [pieces[0], swapped(pieces[1], "tp", 1), far_heads, swapped(far_heads, "tp", 1)]
    far_weight = swapped(out_weight, "tp", far)
    mats = [out_weight, swapped(out_weight, "tp", 1), far_weight, swapped(far_weight, "tp", 1)]
    shares = project(parts, mats)
    mixer = shares[0]
    for k in range(1, lines // 2):
        mixer += swapped(shares[k], "tp", 2 * CORES * k).astype(F32)

    middle = lines // 2
    sums = []
    for name, group in (("N", blocks[:middle]), ("F", blocks[middle:])):
        picked = pick(group, experts_all, capacity)
        maps = weight_maps(group, experts_all, capacity)
        arrived = [picked[0]] + [swapped(picked[k], "ep", k) for k in range(1, ep)]
        done, other_mats = expert(arrived, own_mats, other_mats, name == "N")
        returned = [done[0]] + [swapped(done[k], "ep", k) for k in range(1, ep)]
        sums += combine(maps, returned, len(group), name == "N")
    moe = sums[0]
    for k in range(1, lines):
        moe += swapped(sums[k], "tp", CORES * k).astype(F32)
    return (mixer.astype(BF), moe.astype(BF))


def solution(mesh):
    in_specs = (
        P("ep", "tp"),
        P("ep", None),
        P("ep", None),
        P("tp"),
        P("tp", None),
        P(("ep", "tp"), None),
        P(),
        P(("ep", "tp"), None),
        P(("ep", "tp"), None),
        P("ep", None, "tp"),
        P("ep", None, "tp"),
        P("ep", "tp", None),
    )
    out_specs = (P(("ep", "tp"), None), P(("ep", "tp"), None))
    return jax.shard_map(body, mesh=mesh, in_specs=in_specs, out_specs=out_specs, check_vma=False)
```

```python
import functools

import jax
import jax.numpy as jnp
from jax import lax
from jax.experimental import pallas as pl
from jax.experimental.pallas import tpu as pltpu
from jax.sharding import PartitionSpec as P


HEADS = 16
KV_HEADS = 2
HEAD_DIM = 64
WINDOW = 128
TOP = 2
CORES = 2


big_negative = -1e30
norm_eps = 1e-05
BF = jnp.bfloat16
F32 = jnp.float32
VMEM = pl.BlockSpec(memory_space=pltpu.VMEM)
SMEM = pl.BlockSpec(memory_space=pltpu.SMEM)
HBM = pl.BlockSpec(memory_space=pltpu.HBM)


def swapped(value, axis, mask):
    count = lax.axis_size(axis)
    return lax.ppermute(value, axis, [(i, i ^ mask) for i in range(count)])


def small(mib):
    return pltpu.CompilerParams(vmem_limit_bytes=mib << 20)


def fetch(sources, targets, sems):
    copies = [pltpu.make_async_copy(s, t, sems.at[i]) for i, (s, t) in enumerate(zip(sources, targets))]
    for copy in copies:
        copy.start()
    return copies


def far_away(value):
    return value if value.size == 1 else pltpu.with_memory_space_constraint(value, pltpu.HBM)


def cost(flops, moved):
    return pl.CostEstimate(flops=int(flops), bytes_accessed=int(moved), transcendentals=0)


def nt(a, b):
    return lax.dot_general(a, b, (((1,), (1,)), ((), ())), preferred_element_type=F32)


def relative(i, groups_z):
    return 2 * CORES * (i % groups_z) + CORES * (i // groups_z)


def attend_kernel(where_ref, sink_ref, q_hbm, k_hbm, v_hbm, early_ref, other_ref, *refs):
    out_refs, (q_ref, kv_ref, k_ext, v_ext, sems) = refs[:2], refs[2:]
    blocks, cols = q_ref.shape[0] // WINDOW, q_ref.shape[1]
    groups_z = blocks // 2
    owners = [where_ref[0] ^ relative(i, groups_z) for i in range(blocks)]
    starts = [pl.multiple_of(owner * WINDOW, WINDOW) for owner in owners]
    copies = fetch(
        [k_hbm, v_hbm] + [q_hbm.at[pl.ds(start, WINDOW)] for start in starts],
        [kv_ref.at[0], kv_ref.at[1]] + [q_ref.at[pl.ds(i * WINDOW, WINDOW)] for i in range(blocks)],
        sems,
    )
    heads_here = cols // HEAD_DIM
    key_head = where_ref[1]
    width = KV_HEADS * HEAD_DIM

    def own(values):
        parts = [values[:, h * HEAD_DIM : (h + 1) * HEAD_DIM] for h in range(KV_HEADS)]
        picked = parts[0]
        for h in range(1, KV_HEADS):
            picked = jnp.where(key_head == h, parts[h], picked)
        return picked

    k_ext[...] = jnp.zeros_like(k_ext)
    v_ext[:, :, :cols] = jnp.zeros((heads_here, v_ext.shape[1], cols), BF)
    v_ext[:, :, cols:] = jnp.ones((heads_here, v_ext.shape[1], cols), BF)
    early_k, early_v = own(early_ref[:, :width]), own(early_ref[:, width:])
    for h in range(heads_here):
        place = slice(h * HEAD_DIM, (h + 1) * HEAD_DIM)
        k_ext[h, :WINDOW, place] = early_k
        v_ext[h, :WINDOW, place] = early_v
    for copy in copies:
        copy.wait()
    own_k, own_v = own(kv_ref[0]), own(kv_ref[1])
    for h in range(heads_here):
        place = slice(h * HEAD_DIM, (h + 1) * HEAD_DIM)
        k_ext[h, WINDOW:, place] = own_k
        v_ext[h, WINDOW:, place] = own_v

    row = lax.broadcasted_iota(jnp.int32, (WINDOW, 2 * WINDOW), 0)
    col = lax.broadcasted_iota(jnp.int32, (WINDOW, 2 * WINDOW), 1)
    near = jnp.logical_and(col > row, col <= row + WINDOW)
    tail = other_ref[blocks * WINDOW :, :].astype(F32)
    other_sinks = tail[0:1, :] + tail[1:2, :] + tail[2:3, :]
    for i in range(blocks):
        no_past = jnp.logical_and(owners[i] == 0, where_ref[2] == 0)
        allowed = jnp.logical_and(near, col >= jnp.where(no_past, WINDOW, 0))
        window = pl.ds(starts[i], 2 * WINDOW)
        here = slice(i * WINDOW, (i + 1) * WINDOW)
        out_ref, place = out_refs[i // groups_z], (i % groups_z) * WINDOW
        for core, q_rows in enumerate((q_ref, other_ref)):
            q = q_rows[here, :] * HEAD_DIM ** (-0.5)
            mixed = None
            for h in range(heads_here):
                sink = sink_ref[h] if core == 0 else other_sinks[:, h : h + 1]
                scores = jnp.where(allowed, nt(q, k_ext[h, window, :]), big_negative)
                top = jnp.maximum(jnp.max(scores, -1, keepdims=True), sink)
                powers = jnp.exp(scores - top).astype(BF)
                both = jnp.dot(powers, v_ext[h, window, :], preferred_element_type=F32)
                part = both[:, :cols] / (both[:, cols:] + jnp.exp(sink - top))
                mixed = part if mixed is None else mixed + part
            out_ref[place : place + WINDOW, core * cols : (core + 1) * cols] = mixed.astype(BF)


def attend(queries, other_queries, key_rows, value_rows, sink_logits, earlier):
    total, cols = queries.shape
    assert total // lax.axis_size("tp") == WINDOW
    tp = lax.axis_index("tp")
    key_head = tp * sink_logits.shape[0] // (HEADS // KV_HEADS)
    place = jnp.stack([tp, key_head, lax.axis_index("ep")]).astype(jnp.int32)
    blocks = total // WINDOW // CORES
    return pl.pallas_call(
        attend_kernel,
        in_specs=[SMEM, SMEM] + [HBM] * 3 + [VMEM] * 2,
        out_specs=[VMEM] * 2,
        out_shape=[jax.ShapeDtypeStruct((blocks // 2 * WINDOW, CORES * cols), BF)] * 2,
        scratch_shapes=[
            pltpu.VMEM((blocks * WINDOW, cols), BF),
            pltpu.VMEM((2,) + key_rows.shape, BF),
            pltpu.VMEM((cols // HEAD_DIM, total + WINDOW, cols), BF),
            pltpu.VMEM((cols // HEAD_DIM, total + WINDOW, 2 * cols), BF),
            pltpu.SemaphoreType.DMA((2 + blocks,)),
        ],
        cost_estimate=cost(4e9, 2e6),
        compiler_params=small(8),
        name="attend",
    )(place, far_away(sink_logits), *map(far_away, (queries, key_rows, value_rows)), earlier, other_queries)


def project_kernel(*refs):
    parts, mats, outs = refs[:2], refs[2:6], refs[6:]
    rows = outs[0].shape[0]
    depth, width = mats[0].shape
    tile = min(512, width)
    for n in range(0, width, tile):
        total = None
        for i, mat in enumerate(mats):
            left = parts[i // CORES][:, i % CORES * depth : (i % CORES + 1) * depth]
            term = jnp.dot(left, mat[:, n : n + tile], preferred_element_type=F32)
            total = term if total is None else total + term
        for i, out in enumerate(outs):
            out[:, n : n + tile] = total[i * rows : (i + 1) * rows].astype(out.dtype)


def project(parts, mats):
    rows = parts[0].shape[0]
    width = mats[0].shape[1]
    groups = rows // WINDOW
    out = [jax.ShapeDtypeStruct((WINDOW, width), F32 if i == 0 else BF) for i in range(groups)]
    return pl.pallas_call(
        project_kernel,
        in_specs=[VMEM] * 6,
        out_specs=[VMEM] * groups,
        out_shape=out,
        cost_estimate=cost(2e9, 4e6),
        compiler_params=small(12),
        name="project",
    )(*parts, *mats)


def norm_kernel(experts, where_ref, sink_ref, *refs):
    sources, q_hbm, (out_ref, last_ref, q_ref), refs = refs[:6], refs[6], refs[7:10], refs[10:]
    targets, sems = refs[:4], refs[4]
    x_ref, gain_ref, routes_ref, weight_ref = targets
    cols = sources[4].shape[1]
    end = pl.ds(sources[4].shape[0] - WINDOW, WINDOW)
    blocks = q_ref.shape[0] // WINDOW
    starts = [
        pl.multiple_of((where_ref[0] ^ 1 ^ relative(i, blocks // 2)) * WINDOW, WINDOW) for i in range(blocks)
    ]
    copies = fetch(
        list(sources[:4])
        + [s.at[end] for s in sources[4:]]
        + [q_hbm.at[pl.ds(start, WINDOW)] for start in starts],
        list(targets)
        + [last_ref.at[:, i * cols : (i + 1) * cols] for i in range(2)]
        + [q_ref.at[pl.ds(i * WINDOW, WINDOW)] for i in range(blocks)],
        sems,
    )
    lane = lax.broadcasted_iota(jnp.int32, (16, q_ref.shape[1]), 1)
    row = lax.broadcasted_iota(jnp.int32, (16, q_ref.shape[1]), 0)
    rest = jnp.zeros(lane.shape, F32)
    for h in range(q_ref.shape[1] // HEAD_DIM):
        rest = jnp.where(lane == h, sink_ref[h], rest)
    tail = jnp.zeros(lane.shape, F32)
    for i in range(3):
        part = rest.astype(BF).astype(F32)
        tail = jnp.where(row == i, part, tail)
        rest = rest - part
    q_ref[blocks * WINDOW :, :] = tail.astype(BF)
    for copy in copies:
        copy.wait()
    width = x_ref.shape[1]
    values = x_ref[...].astype(F32)
    center = values - jnp.mean(values, -1, keepdims=True)
    spread = jnp.mean(center * center, -1, keepdims=True)
    out_ref[:, :width] = (center * lax.rsqrt(spread + norm_eps) * gain_ref[...]).astype(BF)
    lane = lax.broadcasted_iota(jnp.int32, (128, x_ref.shape[0]), 0)
    expert = jnp.where(lane < experts, lane, lane - experts)
    weight = jnp.zeros(lane.shape, F32)
    for k in range(TOP):
        weight += jnp.where(routes_ref[k : k + 1, :] == expert, weight_ref[k : k + 1, :], 0.0)
    high = weight.astype(BF).astype(F32)
    table = jnp.where(lane < experts, high, jnp.where(lane < 2 * experts, weight - high, 0.0))
    out_ref[:, width:] = table.T.astype(BF)


def normed_rows(moe_rows, moe_gain, routes, route_weight, experts, key_rows, value_rows, queries, sink_logits):
    rows, width = moe_rows.shape
    cols = key_rows.shape[1]
    total, q_cols = queries.shape
    blocks = total // WINDOW // CORES
    args = (moe_rows, moe_gain[None, :], routes.T, route_weight.T, key_rows, value_rows, queries)
    where = lax.axis_index("tp").astype(jnp.int32)[None]
    return pl.pallas_call(
        functools.partial(norm_kernel, experts),
        in_specs=[SMEM] * 2 + [HBM] * 7,
        out_specs=[VMEM] * 3,
        out_shape=[
            jax.ShapeDtypeStruct((rows, width + 128), BF),
            jax.ShapeDtypeStruct((WINDOW, 2 * cols), BF),
            jax.ShapeDtypeStruct((blocks * WINDOW + 16, q_cols), BF),
        ],
        scratch_shapes=[pltpu.VMEM(a.shape, a.dtype) for a in args[:4]]
        + [pltpu.SemaphoreType.DMA((6 + blocks,))],
        cost_estimate=cost(1e7, 3e5),
        compiler_params=small(8),
        name="normed",
    )(where, far_away(sink_logits), *map(far_away, args))


def slots_of(experts, capacity, blocks, width):
    rows = blocks[0].shape[0]
    tokens = rows * len(blocks)
    table = jnp.concatenate([b[:, width:] for b in blocks], 0).astype(F32).T
    flags = (table > 0).astype(BF)
    source = lax.broadcasted_iota(jnp.int32, (tokens, tokens), 0)
    target = lax.broadcasted_iota(jnp.int32, (tokens, tokens), 1)
    ahead = jnp.logical_and(source < target, source // rows == target // rows).astype(BF)
    position = jnp.dot(flags, ahead, preferred_element_type=F32)
    lane = lax.broadcasted_iota(jnp.int32, (128, tokens), 0)
    base = (lax.broadcasted_iota(jnp.int32, (1, tokens), 1) // rows) * capacity

    def of(expert):
        high = jnp.sum(jnp.where(lane == expert, table, 0.0), 0, keepdims=True)
        low = jnp.sum(jnp.where(lane == expert + experts, table, 0.0), 0, keepdims=True)
        place = jnp.sum(jnp.where(lane == expert, position, 0.0), 0, keepdims=True)
        return jnp.where(high > 0, base + place.astype(jnp.int32), -1), high, low

    return of


def pick_kernel(experts, capacity, ep_ref, *refs):
    lines = len(refs) - experts
    blocks, picked = refs[:lines], refs[lines:]
    slots, width = picked[0].shape
    of = slots_of(experts, capacity, blocks, width)
    slot_id = lax.broadcasted_iota(jnp.int32, (slots, blocks[0].shape[0] * lines), 0)
    values = jnp.concatenate([b[:, :width] for b in blocks], 0)
    for k in range(experts):
        hit = (slot_id == of(ep_ref[0] ^ k)[0]).astype(BF)
        picked[k][...] = jnp.dot(hit, values, preferred_element_type=F32).astype(BF)


def maps_kernel(experts, capacity, ep_ref, *refs):
    lines = len(refs) - 1
    blocks, maps_ref = refs[:lines], refs[lines]
    slots = capacity * lines
    of = slots_of(experts, capacity, blocks, 0)
    slot_id = lax.broadcasted_iota(jnp.int32, (slots, blocks[0].shape[0] * lines), 0)
    for k in range(experts):
        slot, high, low = of(ep_ref[0] ^ k)
        hit = slot_id == slot
        for j, part in enumerate((high, low)):
            maps_ref[2 * k + j] = jnp.where(hit, part, 0.0).T.astype(BF)


def pick(blocks, experts, capacity):
    _, width = blocks[0].shape
    width -= 128
    slots = capacity * len(blocks)
    ep = lax.axis_index("ep").astype(jnp.int32)[None]
    return pl.pallas_call(
        functools.partial(pick_kernel, experts, capacity),
        in_specs=[SMEM] + [VMEM] * len(blocks),
        out_specs=[VMEM] * experts,
        out_shape=[jax.ShapeDtypeStruct((slots, width), BF)] * experts,
        cost_estimate=cost(2e8, 2e6),
        compiler_params=small(12),
        name="pick",
    )(ep, *blocks)


def weight_maps(blocks, experts, capacity):
    rows, width = blocks[0].shape
    slots, tokens = capacity * len(blocks), rows * len(blocks)
    ep = lax.axis_index("ep").astype(jnp.int32)[None]
    tail = pl.BlockSpec((rows, 128), lambda i: (0, width // 128 - 1))
    return pl.pallas_call(
        functools.partial(maps_kernel, experts, capacity),
        grid=(1,),
        in_specs=[SMEM] + [tail] * len(blocks),
        out_specs=pl.BlockSpec((2 * experts, tokens, slots), lambda i: (0, 0, 0)),
        out_shape=jax.ShapeDtypeStruct((2 * experts, tokens, slots), BF),
        cost_estimate=cost(2e7, 1e6),
        compiler_params=small(12),
        name="maps",
    )(ep, *blocks)


def expert_kernel(count, fetching, *refs):
    rows_refs, mats, refs = refs[:count], (refs[count : count + 3], refs[count + 3 : count + 6]), refs[count + 6 :]
    outs, refs = refs[:count], refs[count:]
    copies = [None] * 3
    if fetching:
        held, refs = refs[:3], refs[3:]
        copies = fetch(mats[1], held, refs[3])
        mats = mats[0], held
    all_rows, hidden, total = refs[:3]
    slots, width = rows_refs[0].shape
    units = mats[0][0].shape[1]
    for i in range(count):
        all_rows[i * slots : (i + 1) * slots, :] = rows_refs[i][...]
    tile = 256
    for j, (gate, up, down) in enumerate(mats):
        if fetching and j == 1:
            copies[0].wait()
            copies[1].wait()
        for n in range(0, units, tile):
            cols = slice(n, min(n + tile, units))
            g = jnp.dot(all_rows[...], gate[:, cols], preferred_element_type=F32)
            u = jnp.dot(all_rows[...], up[:, cols], preferred_element_type=F32)
            hidden[j, :, cols] = (g / (1.0 + jnp.exp(-g)) * u).astype(BF)
        if fetching and j == 0:
            for n in range(0, width, tile):
                cols = slice(n, n + tile)
                total[:, cols] = jnp.dot(hidden[0], down[:, cols], preferred_element_type=F32)
    if fetching:
        copies[2].wait()
    for n in range(0, width, tile):
        cols = slice(n, n + tile)
        if fetching:
            term = total[:, cols]
        else:
            term = jnp.dot(hidden[0], mats[0][2][:, cols], preferred_element_type=F32)
        term += jnp.dot(hidden[1], mats[1][2][:, cols], preferred_element_type=F32)
        for i in range(count):
            outs[i][:, cols] = term[i * slots : (i + 1) * slots].astype(BF)


def expert(row_sets, own_mats, other_mats, fetching):
    count = len(row_sets)
    slots, width = row_sets[0].shape
    units = own_mats[0].shape[1]
    total = count * slots
    out = [jax.ShapeDtypeStruct((slots, width), BF)] * count
    scratch = [
        pltpu.VMEM((total, width), BF),
        pltpu.VMEM((2, total, units), BF),
        pltpu.VMEM((total, width), F32),
    ]
    if fetching:
        out += [jax.ShapeDtypeStruct(m.shape, BF) for m in other_mats]
        scratch.append(pltpu.SemaphoreType.DMA((3,)))
        other_mats = list(map(far_away, other_mats))
    result = pl.pallas_call(
        functools.partial(expert_kernel, count, fetching),
        in_specs=[VMEM] * (count + 3) + [HBM if fetching else VMEM] * 3,
        out_specs=[VMEM] * len(out),
        out_shape=out,
        scratch_shapes=scratch,
        cost_estimate=cost(12 * total * width * units, 12 * width * units),
        compiler_params=small(16),
        name="expert",
    )(*row_sets, *own_mats, *other_mats)
    return result[:count], result[count:] if fetching else other_mats


def combine_kernel(experts, maps_ref, *refs):
    results, outs = refs[:experts], refs[experts:]
    rows, width = outs[0].shape
    tile = min(512, width)
    for n in range(0, width, tile):
        cols = slice(n, n + tile)
        total = None
        for k in range(experts):
            for j in range(2):
                term = jnp.dot(maps_ref[2 * k + j], results[k][:, cols], preferred_element_type=F32)
                total = term if total is None else total + term
        for i, out in enumerate(outs):
            out[:, cols] = total[i * rows : (i + 1) * rows].astype(out.dtype)


def combine(maps, results, lines, kept):
    experts = len(results)
    width = results[0].shape[1]
    rows = maps.shape[1] // lines
    out = [jax.ShapeDtypeStruct((rows, width), F32 if i == 0 and kept else BF) for i in range(lines)]
    return pl.pallas_call(
        functools.partial(combine_kernel, experts),
        in_specs=[VMEM] * (1 + experts),
        out_specs=[VMEM] * lines,
        out_shape=out,
        cost_estimate=cost(5e8, 3e6),
        compiler_params=small(12),
        name="combine",
    )(maps, *results)


def body(
    queries,
    key_rows,
    value_rows,
    sink_logits,
    out_weight,
    moe_rows,
    moe_gain,
    routes,
    route_weight,
    gate_weight,
    up_weight,
    down_weight,
):
    tp, ep = lax.axis_size("tp"), lax.axis_size("ep")
    lines, far = tp // CORES, CORES
    experts_all = gate_weight.shape[0] * ep
    capacity = 3 * moe_rows.shape[0] * TOP // (2 * experts_all)

    own, last, for_other = normed_rows(
        moe_rows, moe_gain, routes, route_weight, experts_all, key_rows, value_rows, queries, sink_logits
    )
    blocks = [own] + [swapped(own, "tp", CORES * k) for k in range(1, lines)]
    other_queries = swapped(for_other, "tp", 1)
    earlier = lax.ppermute(last, "ep", [(i, i + 1) for i in range(ep - 1)])
    own_mats = (gate_weight[0], up_weight[0], down_weight[0])
    other_mats = [swapped(m, "tp", 1) for m in own_mats]

    kept, for_far = attend(queries, other_queries, key_rows, value_rows, sink_logits, earlier)
    parts = [kept, swapped(for_far, "tp", far)]
    far_weight = swapped(out_weight, "tp", far)
    out_mats = [out_weight, swapped(out_weight, "tp", 1), far_weight, swapped(far_weight, "tp", 1)]
    shares = project(parts, out_mats)
    mixer = shares[0]
    for k in range(1, lines // 2):
        mixer += swapped(shares[k], "tp", 2 * CORES * k).astype(F32)

    sums = [None] * lines
    for name, first in (("N", 0), ("F", 1)):
        group = blocks[first::2]
        picked = pick(group, experts_all, capacity)
        maps = weight_maps(group, experts_all, capacity)
        arrived = [picked[0]] + [swapped(picked[k], "ep", k) for k in range(1, ep)]
        done, other_mats = expert(arrived, own_mats, other_mats, name == "N")
        returned = [done[0]] + [swapped(done[k], "ep", k) for k in range(1, ep)]
        sums[first::2] = combine(maps, returned, len(group), name == "N")
    moe = sums[0]
    for k in range(1, lines):
        moe += swapped(sums[k], "tp", CORES * k).astype(F32)
    return (mixer.astype(BF), moe.astype(BF))


def solution(mesh):
    in_specs = (
        P("ep", "tp"),
        P("ep", None),
        P("ep", None),
        P("tp"),
        P("tp", None),
        P(("ep", "tp"), None),
        P(),
        P(("ep", "tp"), None),
        P(("ep", "tp"), None),
        P("ep", None, "tp"),
        P("ep", None, "tp"),
        P("ep", "tp", None),
    )
    out_specs = (P(("ep", "tp"), None), P(("ep", "tp"), None))
    return jax.shard_map(body, mesh=mesh, in_specs=in_specs, out_specs=out_specs, check_vma=False)
```

```python
import functools

import jax
import jax.numpy as jnp
from jax import lax
from jax.experimental import pallas as pl
from jax.experimental.pallas import tpu as pltpu
from jax.sharding import PartitionSpec as P


HEADS = 16
KV_HEADS = 2
HEAD_DIM = 64
WINDOW = 128
TOP = 2
CORES = 2


big_negative = -1e30
norm_eps = 1e-05
BF = jnp.bfloat16
F32 = jnp.float32
VMEM = pl.BlockSpec(memory_space=pltpu.VMEM)
SMEM = pl.BlockSpec(memory_space=pltpu.SMEM)
HBM = pl.BlockSpec(memory_space=pltpu.HBM)


def swapped(value, axis, mask):
    count = lax.axis_size(axis)
    return lax.ppermute(value, axis, [(i, i ^ mask) for i in range(count)])


def small(mib):
    return pltpu.CompilerParams(vmem_limit_bytes=mib << 20)


def fetch(sources, targets, sems):
    copies = [pltpu.make_async_copy(s, t, sems.at[i]) for i, (s, t) in enumerate(zip(sources, targets))]
    for copy in copies:
        copy.start()
    return copies


def far_away(value):
    return value if value.size == 1 else pltpu.with_memory_space_constraint(value, pltpu.HBM)


def cost(flops, moved):
    return pl.CostEstimate(flops=int(flops), bytes_accessed=int(moved), transcendentals=0)


def nt(a, b):
    return lax.dot_general(a, b, (((1,), (1,)), ((), ())), preferred_element_type=F32)


def relative(i, groups_z):
    return 2 * CORES * (i % groups_z) + CORES * (i // groups_z)


def attend_kernel(where_ref, sink_ref, q_hbm, k_hbm, v_hbm, early_ref, other_ref, *refs):
    out_refs, (q_ref, kv_ref, k_ext, v_ext, sems) = refs[:2], refs[2:]
    blocks, cols = q_ref.shape[0] // WINDOW, q_ref.shape[1]
    groups_z = blocks // 2
    owners = [where_ref[0] ^ relative(i, groups_z) for i in range(blocks)]
    starts = [pl.multiple_of(owner * WINDOW, WINDOW) for owner in owners]
    copies = fetch(
        [k_hbm, v_hbm] + [q_hbm.at[pl.ds(start, WINDOW)] for start in starts],
        [kv_ref.at[0], kv_ref.at[1]] + [q_ref.at[pl.ds(i * WINDOW, WINDOW)] for i in range(blocks)],
        sems,
    )
    heads_here = cols // HEAD_DIM
    key_head = where_ref[1]
    width = KV_HEADS * HEAD_DIM

    def own(values):
        parts = [values[:, h * HEAD_DIM : (h + 1) * HEAD_DIM] for h in range(KV_HEADS)]
        picked = parts[0]
        for h in range(1, KV_HEADS):
            picked = jnp.where(key_head == h, parts[h], picked)
        return picked

    k_ext[...] = jnp.zeros_like(k_ext)
    v_ext[:, :, :cols] = jnp.zeros((heads_here, v_ext.shape[1], cols), BF)
    v_ext[:, :, cols:] = jnp.ones((heads_here, v_ext.shape[1], cols), BF)
    early_k, early_v = own(early_ref[:, :width]), own(early_ref[:, width:])
    for h in range(heads_here):
        place = slice(h * HEAD_DIM, (h + 1) * HEAD_DIM)
        k_ext[h, :WINDOW, place] = early_k
        v_ext[h, :WINDOW, place] = early_v
    for copy in copies:
        copy.wait()
    own_k, own_v = own(kv_ref[0]), own(kv_ref[1])
    for h in range(heads_here):
        place = slice(h * HEAD_DIM, (h + 1) * HEAD_DIM)
        k_ext[h, WINDOW:, place] = own_k
        v_ext[h, WINDOW:, place] = own_v

    row = lax.broadcasted_iota(jnp.int32, (WINDOW, 2 * WINDOW), 0)
    col = lax.broadcasted_iota(jnp.int32, (WINDOW, 2 * WINDOW), 1)
    near = jnp.logical_and(col > row, col <= row + WINDOW)
    tail = other_ref[blocks * WINDOW :, :].astype(F32)
    other_sinks = tail[0:1, :] + tail[1:2, :] + tail[2:3, :]
    for i in range(blocks):
        no_past = jnp.logical_and(owners[i] == 0, where_ref[2] == 0)
        allowed = jnp.logical_and(near, col >= jnp.where(no_past, WINDOW, 0))
        window = pl.ds(starts[i], 2 * WINDOW)
        here = slice(i * WINDOW, (i + 1) * WINDOW)
        out_ref, place = out_refs[i // groups_z], (i % groups_z) * WINDOW
        for core, q_rows in enumerate((q_ref, other_ref)):
            q = q_rows[here, :] * HEAD_DIM ** (-0.5)
            mixed = None
            for h in range(heads_here):
                sink = sink_ref[h] if core == 0 else other_sinks[:, h : h + 1]
                scores = jnp.where(allowed, nt(q, k_ext[h, window, :]), big_negative)
                top = jnp.maximum(jnp.max(scores, -1, keepdims=True), sink)
                powers = jnp.exp(scores - top).astype(BF)
                both = jnp.dot(powers, v_ext[h, window, :], preferred_element_type=F32)
                part = both[:, :cols] / (both[:, cols:] + jnp.exp(sink - top))
                mixed = part if mixed is None else mixed + part
            out_ref[place : place + WINDOW, core * cols : (core + 1) * cols] = mixed.astype(BF)


def attend(queries, other_queries, key_rows, value_rows, sink_logits, earlier):
    total, cols = queries.shape
    assert total // lax.axis_size("tp") == WINDOW
    tp = lax.axis_index("tp")
    key_head = tp * sink_logits.shape[0] // (HEADS // KV_HEADS)
    place = jnp.stack([tp, key_head, lax.axis_index("ep")]).astype(jnp.int32)
    blocks = total // WINDOW // CORES
    return pl.pallas_call(
        attend_kernel,
        in_specs=[SMEM, SMEM] + [HBM] * 3 + [VMEM] * 2,
        out_specs=[VMEM] * 2,
        out_shape=[jax.ShapeDtypeStruct((blocks // 2 * WINDOW, CORES * cols), BF)] * 2,
        scratch_shapes=[
            pltpu.VMEM((blocks * WINDOW, cols), BF),
            pltpu.VMEM((2,) + key_rows.shape, BF),
            pltpu.VMEM((cols // HEAD_DIM, total + WINDOW, cols), BF),
            pltpu.VMEM((cols // HEAD_DIM, total + WINDOW, 2 * cols), BF),
            pltpu.SemaphoreType.DMA((2 + blocks,)),
        ],
        cost_estimate=cost(4e9, 2e6),
        compiler_params=small(8),
        name="attend",
    )(place, far_away(sink_logits), *map(far_away, (queries, key_rows, value_rows)), earlier, other_queries)


def project_kernel(*refs):
    parts, mats, outs = refs[:2], refs[2:6], refs[6:]
    rows = outs[0].shape[0]
    depth, width = mats[0].shape
    tile = min(512, width)
    for n in range(0, width, tile):
        total = None
        for i, mat in enumerate(mats):
            left = parts[i // CORES][:, i % CORES * depth : (i % CORES + 1) * depth]
            term = jnp.dot(left, mat[:, n : n + tile], preferred_element_type=F32)
            total = term if total is None else total + term
        for i, out in enumerate(outs):
            out[:, n : n + tile] = total[i * rows : (i + 1) * rows].astype(out.dtype)


def project(parts, mats):
    rows = parts[0].shape[0]
    width = mats[0].shape[1]
    groups = rows // WINDOW
    out = [jax.ShapeDtypeStruct((WINDOW, width), F32 if i == 0 else BF) for i in range(groups)]
    return pl.pallas_call(
        project_kernel,
        in_specs=[VMEM] * 6,
        out_specs=[VMEM] * groups,
        out_shape=out,
        cost_estimate=cost(2e9, 4e6),
        compiler_params=small(12),
        name="project",
    )(*parts, *mats)


def norm_kernel(experts, where_ref, sink_ref, *refs):
    sources, q_hbm, (out_ref, last_ref, q_ref), refs = refs[:6], refs[6], refs[7:10], refs[10:]
    targets, sems = refs[:4], refs[4]
    x_ref, gain_ref, routes_ref, weight_ref = targets
    cols = sources[4].shape[1]
    end = pl.ds(sources[4].shape[0] - WINDOW, WINDOW)
    blocks = q_ref.shape[0] // WINDOW
    starts = [
        pl.multiple_of((where_ref[0] ^ 1 ^ relative(i, blocks // 2)) * WINDOW, WINDOW) for i in range(blocks)
    ]
    copies = fetch(
        list(sources[:4])
        + [s.at[end] for s in sources[4:]]
        + [q_hbm.at[pl.ds(start, WINDOW)] for start in starts],
        list(targets)
        + [last_ref.at[:, i * cols : (i + 1) * cols] for i in range(2)]
        + [q_ref.at[pl.ds(i * WINDOW, WINDOW)] for i in range(blocks)],
        sems,
    )
    lane = lax.broadcasted_iota(jnp.int32, (16, q_ref.shape[1]), 1)
    row = lax.broadcasted_iota(jnp.int32, (16, q_ref.shape[1]), 0)
    rest = jnp.zeros(lane.shape, F32)
    for h in range(q_ref.shape[1] // HEAD_DIM):
        rest = jnp.where(lane == h, sink_ref[h], rest)
    tail = jnp.zeros(lane.shape, F32)
    for i in range(3):
        part = rest.astype(BF).astype(F32)
        tail = jnp.where(row == i, part, tail)
        rest = rest - part
    q_ref[blocks * WINDOW :, :] = tail.astype(BF)
    for copy in copies:
        copy.wait()
    width = x_ref.shape[1]
    values = x_ref[...].astype(F32)
    center = values - jnp.mean(values, -1, keepdims=True)
    spread = jnp.mean(center * center, -1, keepdims=True)
    out_ref[:, :width] = (center * lax.rsqrt(spread + norm_eps) * gain_ref[...]).astype(BF)
    lane = lax.broadcasted_iota(jnp.int32, (128, x_ref.shape[0]), 0)
    expert = jnp.where(lane < experts, lane, lane - experts)
    weight = jnp.zeros(lane.shape, F32)
    for k in range(TOP):
        weight += jnp.where(routes_ref[k : k + 1, :] == expert, weight_ref[k : k + 1, :], 0.0)
    high = weight.astype(BF).astype(F32)
    table = jnp.where(lane < experts, high, jnp.where(lane < 2 * experts, weight - high, 0.0))
    out_ref[:, width:] = table.T.astype(BF)


def normed_rows(moe_rows, moe_gain, routes, route_weight, experts, key_rows, value_rows, queries, sink_logits):
    rows, width = moe_rows.shape
    cols = key_rows.shape[1]
    total, q_cols = queries.shape
    blocks = total // WINDOW // CORES
    args = (moe_rows, moe_gain[None, :], routes.T, route_weight.T, key_rows, value_rows, queries)
    where = lax.axis_index("tp").astype(jnp.int32)[None]
    return pl.pallas_call(
        functools.partial(norm_kernel, experts),
        in_specs=[SMEM] * 2 + [HBM] * 7,
        out_specs=[VMEM] * 3,
        out_shape=[
            jax.ShapeDtypeStruct((rows, width + 128), BF),
            jax.ShapeDtypeStruct((WINDOW, 2 * cols), BF),
            jax.ShapeDtypeStruct((blocks * WINDOW + 16, q_cols), BF),
        ],
        scratch_shapes=[pltpu.VMEM(a.shape, a.dtype) for a in args[:4]]
        + [pltpu.SemaphoreType.DMA((6 + blocks,))],
        cost_estimate=cost(1e7, 3e5),
        compiler_params=small(8),
        name="normed",
    )(where, far_away(sink_logits), *map(far_away, args))


def slots_of(experts, capacity, blocks, width):
    rows = blocks[0].shape[0]
    tokens = rows * len(blocks)
    table = jnp.concatenate([b[:, width:] for b in blocks], 0).astype(F32).T
    flags = (table > 0).astype(BF)
    source = lax.broadcasted_iota(jnp.int32, (tokens, tokens), 0)
    target = lax.broadcasted_iota(jnp.int32, (tokens, tokens), 1)
    ahead = jnp.logical_and(source < target, source // rows == target // rows).astype(BF)
    position = jnp.dot(flags, ahead, preferred_element_type=F32)
    lane = lax.broadcasted_iota(jnp.int32, (128, tokens), 0)
    base = (lax.broadcasted_iota(jnp.int32, (1, tokens), 1) // rows) * capacity

    def of(expert):
        high = jnp.sum(jnp.where(lane == expert, table, 0.0), 0, keepdims=True)
        low = jnp.sum(jnp.where(lane == expert + experts, table, 0.0), 0, keepdims=True)
        place = jnp.sum(jnp.where(lane == expert, position, 0.0), 0, keepdims=True)
        return jnp.where(high > 0, base + place.astype(jnp.int32), -1), high, low

    return of


def pick_kernel(experts, capacity, ep_ref, *refs):
    lines = len(refs) - experts
    blocks, picked = refs[:lines], refs[lines:]
    slots, width = picked[0].shape
    of = slots_of(experts, capacity, blocks, width)
    slot_id = lax.broadcasted_iota(jnp.int32, (slots, blocks[0].shape[0] * lines), 0)
    values = jnp.concatenate([b[:, :width] for b in blocks], 0)
    for k in range(experts):
        hit = (slot_id == of(ep_ref[0] ^ k)[0]).astype(BF)
        picked[k][...] = jnp.dot(hit, values, preferred_element_type=F32).astype(BF)


def maps_kernel(experts, capacity, ep_ref, *refs):
    lines = len(refs) - 1
    blocks, maps_ref = refs[:lines], refs[lines]
    slots = capacity * lines
    of = slots_of(experts, capacity, blocks, 0)
    slot_id = lax.broadcasted_iota(jnp.int32, (slots, blocks[0].shape[0] * lines), 0)
    for k in range(experts):
        slot, high, low = of(ep_ref[0] ^ k)
        hit = slot_id == slot
        for j, part in enumerate((high, low)):
            maps_ref[2 * k + j] = jnp.where(hit, part, 0.0).T.astype(BF)


def pick(blocks, experts, capacity):
    _, width = blocks[0].shape
    width -= 128
    slots = capacity * len(blocks)
    ep = lax.axis_index("ep").astype(jnp.int32)[None]
    return pl.pallas_call(
        functools.partial(pick_kernel, experts, capacity),
        in_specs=[SMEM] + [VMEM] * len(blocks),
        out_specs=[VMEM] * experts,
        out_shape=[jax.ShapeDtypeStruct((slots, width), BF)] * experts,
        cost_estimate=cost(2e8, 2e6),
        compiler_params=small(12),
        name="pick",
    )(ep, *blocks)


def weight_maps(blocks, experts, capacity):
    rows, width = blocks[0].shape
    slots, tokens = capacity * len(blocks), rows * len(blocks)
    ep = lax.axis_index("ep").astype(jnp.int32)[None]
    tail = pl.BlockSpec((rows, 128), lambda i: (0, width // 128 - 1))
    return pl.pallas_call(
        functools.partial(maps_kernel, experts, capacity),
        grid=(1,),
        in_specs=[SMEM] + [tail] * len(blocks),
        out_specs=pl.BlockSpec((2 * experts, tokens, slots), lambda i: (0, 0, 0)),
        out_shape=jax.ShapeDtypeStruct((2 * experts, tokens, slots), BF),
        cost_estimate=cost(2e7, 1e6),
        compiler_params=small(12),
        name="maps",
    )(ep, *blocks)


def expert_kernel(count, fetching, *refs):
    rows_refs, mats, refs = refs[:count], (refs[count : count + 3], refs[count + 3 : count + 6]), refs[count + 6 :]
    outs, refs = refs[:count], refs[count:]
    copies = [None] * 3
    if fetching:
        held, refs = refs[:2], refs[2:]
        copies = fetch(mats[1][:2], held, refs[3])
        mats = mats[0], (*held, mats[1][2])
    all_rows, hidden, total = refs[:3]
    slots, width = rows_refs[0].shape
    units = mats[0][0].shape[1]
    for i in range(count):
        all_rows[i * slots : (i + 1) * slots, :] = rows_refs[i][...]
    tile = 256
    for j, (gate, up, down) in enumerate(mats):
        if fetching and j == 1:
            copies[0].wait()
            copies[1].wait()
        for n in range(0, units, tile):
            cols = slice(n, min(n + tile, units))
            g = jnp.dot(all_rows[...], gate[:, cols], preferred_element_type=F32)
            u = jnp.dot(all_rows[...], up[:, cols], preferred_element_type=F32)
            hidden[j, :, cols] = (g / (1.0 + jnp.exp(-g)) * u).astype(BF)
        if fetching and j == 0:
            for n in range(0, width, tile):
                cols = slice(n, n + tile)
                total[:, cols] = jnp.dot(hidden[0], down[:, cols], preferred_element_type=F32)
    for n in range(0, width, tile):
        cols = slice(n, n + tile)
        if fetching:
            term = total[:, cols]
        else:
            term = jnp.dot(hidden[0], mats[0][2][:, cols], preferred_element_type=F32)
        term += jnp.dot(hidden[1], mats[1][2][:, cols], preferred_element_type=F32)
        for i in range(count):
            outs[i][:, cols] = term[i * slots : (i + 1) * slots].astype(BF)


def expert(row_sets, own_mats, other_mats, fetching):
    count = len(row_sets)
    slots, width = row_sets[0].shape
    units = own_mats[0].shape[1]
    total = count * slots
    out = [jax.ShapeDtypeStruct((slots, width), BF)] * count
    scratch = [
        pltpu.VMEM((total, width), BF),
        pltpu.VMEM((2, total, units), BF),
        pltpu.VMEM((total, width), F32),
    ]
    if fetching:
        out += [jax.ShapeDtypeStruct(m.shape, BF) for m in other_mats[:2]]
        scratch.append(pltpu.SemaphoreType.DMA((2,)))
        other_mats = [*map(far_away, other_mats[:2]), other_mats[2]]
    result = pl.pallas_call(
        functools.partial(expert_kernel, count, fetching),
        in_specs=[VMEM] * (count + 3) + [HBM if fetching else VMEM] * 2 + [VMEM],
        out_specs=[VMEM] * len(out),
        out_shape=out,
        scratch_shapes=scratch,
        cost_estimate=cost(12 * total * width * units, 12 * width * units),
        compiler_params=small(16),
        name="expert",
    )(*row_sets, *own_mats, *other_mats)
    return result[:count], [*result[count:], other_mats[2]] if fetching else other_mats


def combine_kernel(experts, maps_ref, *refs):
    results, outs = refs[:experts], refs[experts:]
    rows, width = outs[0].shape
    tile = min(512, width)
    for n in range(0, width, tile):
        cols = slice(n, n + tile)
        total = None
        for k in range(experts):
            for j in range(2):
                term = jnp.dot(maps_ref[2 * k + j], results[k][:, cols], preferred_element_type=F32)
                total = term if total is None else total + term
        for i, out in enumerate(outs):
            out[:, cols] = total[i * rows : (i + 1) * rows].astype(out.dtype)


def combine(maps, results, lines, kept):
    experts = len(results)
    width = results[0].shape[1]
    rows = maps.shape[1] // lines
    out = [jax.ShapeDtypeStruct((rows, width), F32 if i == 0 and kept else BF) for i in range(lines)]
    return pl.pallas_call(
        functools.partial(combine_kernel, experts),
        in_specs=[VMEM] * (1 + experts),
        out_specs=[VMEM] * lines,
        out_shape=out,
        cost_estimate=cost(5e8, 3e6),
        compiler_params=small(12),
        name="combine",
    )(maps, *results)


def body(
    queries,
    key_rows,
    value_rows,
    sink_logits,
    out_weight,
    moe_rows,
    moe_gain,
    routes,
    route_weight,
    gate_weight,
    up_weight,
    down_weight,
):
    tp, ep = lax.axis_size("tp"), lax.axis_size("ep")
    lines, far = tp // CORES, CORES
    experts_all = gate_weight.shape[0] * ep
    capacity = 3 * moe_rows.shape[0] * TOP // (2 * experts_all)

    own, last, for_other = normed_rows(
        moe_rows, moe_gain, routes, route_weight, experts_all, key_rows, value_rows, queries, sink_logits
    )
    blocks = [own] + [swapped(own, "tp", CORES * k) for k in range(1, lines)]
    other_queries = swapped(for_other, "tp", 1)
    earlier = lax.ppermute(last, "ep", [(i, i + 1) for i in range(ep - 1)])
    own_mats = (gate_weight[0], up_weight[0], down_weight[0])
    other_mats = [swapped(m, "tp", 1) for m in own_mats]

    kept, for_far = attend(queries, other_queries, key_rows, value_rows, sink_logits, earlier)
    parts = [kept, swapped(for_far, "tp", far)]
    far_weight = swapped(out_weight, "tp", far)
    out_mats = [out_weight, swapped(out_weight, "tp", 1), far_weight, swapped(far_weight, "tp", 1)]
    shares = project(parts, out_mats)
    mixer = shares[0]
    for k in range(1, lines // 2):
        mixer += swapped(shares[k], "tp", 2 * CORES * k).astype(F32)

    sums = [None] * lines
    for name, first in (("N", 0), ("F", 1)):
        group = blocks[first::2]
        picked = pick(group, experts_all, capacity)
        maps = weight_maps(group, experts_all, capacity)
        arrived = [picked[0]] + [swapped(picked[k], "ep", k) for k in range(1, ep)]
        done, other_mats = expert(arrived, own_mats, other_mats, name == "N")
        returned = [done[0]] + [swapped(done[k], "ep", k) for k in range(1, ep)]
        sums[first::2] = combine(maps, returned, len(group), name == "N")
    moe = sums[0]
    for k in range(1, lines):
        moe += swapped(sums[k], "tp", CORES * k).astype(F32)
    return (mixer.astype(BF), moe.astype(BF))


def solution(mesh):
    in_specs = (
        P("ep", "tp"),
        P("ep", None),
        P("ep", None),
        P("tp"),
        P("tp", None),
        P(("ep", "tp"), None),
        P(),
        P(("ep", "tp"), None),
        P(("ep", "tp"), None),
        P("ep", None, "tp"),
        P("ep", None, "tp"),
        P("ep", "tp", None),
    )
    out_specs = (P(("ep", "tp"), None), P(("ep", "tp"), None))
    return jax.shard_map(body, mesh=mesh, in_specs=in_specs, out_specs=out_specs, check_vma=False)
```
